32 devices in a mesh: kv: 8 (over z, y), tp: 4 (over x, core).
Axes of the slice: x: 2, y: 2, z: 4, core: 2. Of those that a mesh axis runs over, the one named last changes fastest.
Arguments:
- tokens: bfloat16 [8, 2048], P(None, 'kv'), may hold values from -6 to 6
- in_gain: float32 [2048], P('kv'), may hold values from 0.1 to 1.9
- w_query: bfloat16 [2048, 512], P('kv', 'tp'), may hold values from -0.125 to 0.125
- score_bias: float32 [4], P('tp'), as said below
- cache_keys: bfloat16 [8, 8192, 512], P(None, 'kv', 'tp'), may hold values from -8 to 8, as said below
- cache_values: bfloat16 [8, 8192, 512], P(None, 'kv', 'tp'), may hold values from -6 to 6
- lengths: int32 [8], replicated, may hold values from 1024 to 8192, as said below
- head_gain: float32 [512], P('tp'), may hold values from 0.1 to 1.9
- w_out: bfloat16 [512, 2048], P('tp', 'kv'), may hold values from -0.25 to 0.25
Outputs:
- mixed: bfloat16 [8, 2048], P(None, 'kv')
The draws below stay inside these ranges and needn't reach their ends.
Inputs may be any that keep to these rules, and one draw needn't show every extreme that they name: `score_bias`: one value a head, added to every score of that head. `cache_keys`: real-valued key entries. `lengths`: one sequence has all 8192 positions cached.
All inputs are finite; a program needn't handle non-finite values.
Results may differ from the reference program's by a relative error of at most 0.0095.
The reference program's roundings to bfloat16 on the way (of `gained`, `queries`, `weights` and `normed`) count: a program that leaves them out, or rounds other values in their place, can miss the bound.
Values may be sent and summed in bfloat16 or wider, within the bound.
A program may use at most 64 MiB of HBM per device.

```python
import jax
import jax.numpy as jnp
from jax import lax

D = 2048
HEADS = 4
DH = 128
SEQS = 8
POS_DEV = 1024
SEQ_LEN = 8192
N_TP = 4


def draw_score_bias(key, part):
    key_order, key_slow, key_fast = jax.random.split(jax.random.fold_in(key, 11), 3)
    slow_heads = jax.random.permutation(key_order, HEADS) < HEADS // 2
    slow_value = -jnp.log(jnp.float32(SEQ_LEN)) + jax.random.uniform(key_slow, (HEADS,), jnp.float32, -0.6, 0.0)
    fast_value = -jnp.log(jax.random.uniform(key_fast, (HEADS,), jnp.float32, 30.0, 100.0)) - 1.1
    return jnp.where(slow_heads, slow_value, fast_value).astype(jnp.float32)


def draw_cache_keys(key, part):
    key_scale, key_base = jax.random.split(jax.random.fold_in(key, 3))
    spans = SEQ_LEN // 32
    span_scale = jax.random.uniform(key_scale, (SEQS, spans, 1, HEADS, 1), jnp.float32, 0.5, 2.0)
    unit_draw = jnp.clip(jax.random.normal(key_base, (SEQS, spans, 32, HEADS, DH), jnp.float32), -4.0, 4.0)
    return (unit_draw * span_scale).reshape(SEQS, SEQ_LEN, HEADS * DH).astype(jnp.bfloat16)


def draw_lengths(key, part):
    key_lens, key_full = jax.random.split(jax.random.fold_in(key, 7))
    drawn = jax.random.randint(key_lens, (SEQS,), SEQ_LEN // 8, SEQ_LEN + 1)
    chosen = jax.random.randint(key_full, (), 0, SEQS)
    return jnp.where(jnp.arange(SEQS) == chosen, SEQ_LEN, drawn).astype(jnp.int32)


def level_of(rng, dims, cuts, least, largest):
    level, own = 1.0, jax.random.fold_in(rng, 6)
    for dim, parts in cuts:
        heights = jnp.exp(jax.random.uniform(jax.random.fold_in(own, dim), (parts,), jnp.float32, least / len(cuts), largest / len(cuts)))
        level = level * jnp.repeat(heights, dims[dim] // parts).reshape([-1 if axis == dim else 1 for axis in range(len(dims))])
    return level


def bell_draw(stream_key, extent, deviation, reach, shards=(), kind=jnp.bfloat16):
    values = deviation * jax.random.normal(stream_key, extent, jnp.float32)
    if shards:
        values = values * level_of(stream_key, extent, shards, -0.22, 0.18)
    return jnp.clip(values, -reach, reach).astype(kind)


def setup_inputs(seed: int = 0) -> dict:
    key_of = jax.random.split(jax.random.key(seed), 10)
    tokens = bell_draw(key_of[0], (SEQS, D), 1.0, 6.0, ((1, 8),))
    in_gain = jnp.clip(1.0 + 0.18 * jax.random.normal(key_of[1], (D,), jnp.float32), 0.1, 1.9)
    w_query = bell_draw(key_of[2], (D, HEADS * DH), D ** -0.5, 0.125, ((0, 8), (1, 4)))
    score_bias = draw_score_bias(jax.random.fold_in(key_of[9], 71), 0)
    cache_keys = draw_cache_keys(jax.random.fold_in(key_of[9], 71), 0)
    cache_values = bell_draw(key_of[5], (SEQS, SEQ_LEN, HEADS * DH), 1.0, 6.0, ((1, 8), (2, 4)))
    lengths = draw_lengths(jax.random.fold_in(key_of[9], 71), 0)
    head_gain = jnp.clip(1.0 + 0.18 * jax.random.normal(key_of[7], (HEADS * DH,), jnp.float32), 0.1, 1.9)
    w_out = bell_draw(key_of[8], (HEADS * DH, D), (HEADS * DH) ** -0.5, 0.25, ((0, 4), (1, 8)))
    return dict(tokens=tokens, in_gain=in_gain, w_query=w_query, score_bias=score_bias, cache_keys=cache_keys, cache_values=cache_values, lengths=lengths, head_gain=head_gain, w_out=w_out)


EPS = 1e-06

def reference(tokens, in_gain, w_query, score_bias, cache_keys, cache_values, lengths, head_gain, w_out):
    as_float = tokens.astype(jnp.float32)
    gained = (as_float * in_gain).astype(jnp.bfloat16)
    raw_query = jnp.dot(gained, w_query, preferred_element_type=jnp.float32)
    row_scale = lax.rsqrt(lax.optimization_barrier(jnp.mean(as_float * as_float, axis=1)) + EPS)
    queries = (raw_query * row_scale[:, None]).astype(jnp.bfloat16).reshape(SEQS, HEADS, DH)
    segments = SEQ_LEN // POS_DEV

    def per_sequence(fields):
        seq_query, seq_keys, seq_values, seq_len = fields
        keys_f32 = seq_keys.astype(jnp.float32).reshape(SEQ_LEN, HEADS, DH)
        scores = jnp.einsum('hd,lhd->hl', seq_query.astype(jnp.float32), keys_f32) * DH ** (-0.5)
        scores = scores + score_bias[:, None]
        usable = (jnp.arange(SEQ_LEN, dtype=jnp.int32) < seq_len)[None, :]
        log_keep = jnp.where(usable, jax.nn.log_sigmoid(-scores), 0.0)
        segmented = log_keep.reshape(HEADS, segments, POS_DEV)
        suffix = lax.cumsum(segmented, axis=2, reverse=True) - segmented
        gate_log = jax.nn.log_sigmoid(scores).reshape(HEADS, segments, POS_DEV)
        weights = jnp.where(usable.reshape(1, segments, POS_DEV), jnp.exp(gate_log + suffix), 0.0)
        weights = weights.astype(jnp.bfloat16)
        values_f32 = seq_values.astype(jnp.float32).reshape(segments, POS_DEV, HEADS, DH)
        seg_out = jnp.einsum('hnp,nphd->hnd', weights.astype(jnp.float32), values_f32)
        totals = lax.optimization_barrier(jnp.sum(segmented, axis=2))
        later_sum = lax.cumsum(totals, axis=1, reverse=True) - totals
        return lax.optimization_barrier(jnp.sum(seg_out * jnp.exp(later_sum)[..., None], axis=1))
    attended = lax.map(per_sequence, (queries, cache_keys, cache_values, lengths))
    mean_sq = lax.optimization_barrier(jnp.mean(attended * attended, axis=2))
    normed = attended * lax.rsqrt(mean_sq + EPS)[..., None]
    normed = (normed.reshape(SEQS, HEADS * DH) * head_gain).astype(jnp.bfloat16)
    block_width = HEADS * DH // N_TP
    mixed = jnp.zeros((SEQS, D), jnp.float32)
    for block in range(N_TP):
        part_out = jnp.dot(normed[:, block * block_width:(block + 1) * block_width], w_out[block * block_width:(block + 1) * block_width], preferred_element_type=jnp.float32)
        mixed = mixed + lax.optimization_barrier(part_out.astype(jnp.bfloat16)).astype(jnp.float32)
    return mixed.astype(jnp.bfloat16)
```

```python
import functools

import jax
import jax.numpy as jnp
from jax import lax
from jax.experimental import pallas as pl
from jax.experimental.pallas import tpu as pltpu
from jax.sharding import PartitionSpec as P

EPS = 1e-06
LANES = 128
MESH = pl.DeviceIdType.MESH


def each(count, body, first=0):
    if count - first <= 16:
        for i in range(first, count):
            body(i)
    else:
        lax.fori_loop(first, count, lambda i, c: (body(i), c)[1], 0)


def folded(count, body, init):
    if count <= 16:
        for i in range(count):
            init = body(i, init)
        return init
    return lax.fori_loop(0, count, body, init)


def push(axis, me, count, buf, send_sem, recv_sem):
    def copy(i):
        return pltpu.make_async_remote_copy(
            src_ref=buf.at[me],
            dst_ref=buf.at[me],
            send_sem=send_sem.at[i],
            recv_sem=recv_sem.at[i],
            device_id={axis: lax.rem(me + i, count)},
            device_id_type=MESH,
        )

    return copy


def arrival(axis, me, count, buf, send_sem, recv_sem):
    def copy(i):
        slot = lax.rem(me + count - i, count)
        return pltpu.make_async_remote_copy(
            src_ref=buf.at[slot],
            dst_ref=buf.at[slot],
            send_sem=send_sem.at[i],
            recv_sem=recv_sem.at[i],
            device_id={axis: slot},
            device_id_type=MESH,
        )

    return copy


def kernel(
    n_kv, n_tp,
    tok_hbm, gain_hbm, wq_hbm, bias_hbm, keys_hbm, values_hbm, len_hbm, hg_hbm, wo_hbm,
    out_ref,
    tok, gain, wq, bias, keys, values, lens, hg, wo,
    qbuf, obuf, tbuf,
    load_sem, key_sem, value_sem,
    q_send, q_recv, o_send, o_recv, t_send, t_recv,
):
    me = lax.axis_index("kv")
    mine = lax.axis_index("tp")
    seqs, local_len, size = keys.shape
    chunks = local_len // LANES

    small = [
        pltpu.make_async_copy(src, dst, load_sem.at[i])
        for i, (src, dst) in enumerate(
            ((tok_hbm, tok), (gain_hbm, gain), (wq_hbm, wq), (bias_hbm, bias),
             (len_hbm, lens), (hg_hbm, hg), (wo_hbm, wo))
        )
    ]
    for copy in small:
        copy.start()
    barrier = pltpu.get_barrier_semaphore()

    def greet(axis, place, count):
        def body(i):
            pl.semaphore_signal(
                barrier, inc=1, device_id={axis: lax.rem(place + i, count)}, device_id_type=MESH
            )

        each(count, body, 1)

    greet("kv", me, n_kv)
    greet("tp", mine, n_tp)
    pairs = seqs // 2
    key_loads = [
        pltpu.make_async_copy(
            keys_hbm.at[pl.ds(2 * i, 2)], keys.at[pl.ds(2 * i, 2)], key_sem.at[i]
        )
        for i in range(pairs)
    ]
    value_loads = [
        pltpu.make_async_copy(
            values_hbm.at[pl.ds(2 * i, 2)], values.at[pl.ds(2 * i, 2)], value_sem.at[i]
        )
        for i in range(pairs)
    ]
    for copy in key_loads + value_loads:
        copy.start()

    for copy in small[:3]:
        copy.wait()
    as_float = tok[...].astype(jnp.float32)
    gained = (as_float * gain[...]).astype(jnp.bfloat16)
    partial = jnp.dot(gained, wq[...], preferred_element_type=jnp.float32)
    squares = jnp.sum(as_float * as_float, axis=1, keepdims=True)
    qbuf[me, pl.ds(0, seqs)] = partial
    qbuf[me, pl.ds(seqs, seqs)] = jnp.broadcast_to(squares, (seqs, size))
    pl.semaphore_wait(barrier, n_kv - 1 + n_tp - 1)
    q_push = push("kv", me, n_kv, qbuf, q_send, q_recv)
    q_arrival = arrival("kv", me, n_kv, qbuf, q_send, q_recv)
    each(n_kv, lambda i: q_push(i).start(), 1)

    for copy in small[3:]:
        copy.wait()
    row = lax.broadcasted_iota(jnp.int32, (seqs, LANES), 0)
    lane = lax.broadcasted_iota(jnp.int32, (seqs, LANES), 1)
    length = jnp.zeros((seqs, LANES), jnp.int32)
    for b in range(seqs):
        length = jnp.where(row == b, lens[b], length)
    left = length - (me * local_len + lane)
    shift = bias[0]
    from_row = lax.broadcasted_iota(jnp.int32, (LANES, 2 * LANES), 0)
    to_lane = lax.broadcasted_iota(jnp.int32, (LANES, 2 * LANES), 1)
    later_of = jnp.where((from_row >= to_lane) | (to_lane >= LANES), 1.0, 0.0).astype(jnp.bfloat16)
    for copy in key_loads:
        copy.wait()

    each(n_kv, lambda i: q_arrival(i).wait_recv(), 1)
    total = folded(n_kv, lambda i, acc: acc + qbuf[i], jnp.zeros((2 * seqs, size), jnp.float32))
    features = tok.shape[1] * n_kv
    row_scale = lax.rsqrt(total[seqs:] / features + EPS)
    queries = total[:seqs] * row_scale
    queries = queries.astype(jnp.bfloat16).astype(jnp.float32)
    qrow = lax.broadcasted_iota(jnp.int32, (seqs, size), 0)

    scores = None
    for i in range(pairs):
        lhs = jnp.concatenate(
            [jnp.where(qrow == 2 * i + k, queries, 0.0) for k in range(2)], axis=1
        ).astype(jnp.bfloat16)
        rhs = jnp.concatenate([keys[2 * i], keys[2 * i + 1]], axis=1)
        term = lax.dot_general(
            lhs, rhs, (((1,), (1,)), ((), ())), preferred_element_type=jnp.float32
        )
        scores = term if scores is None else scores + term
    scores = scores * size ** (-0.5) + shift

    usable, parts = [], []
    for j in range(chunks):
        s = scores[:, j * LANES : (j + 1) * LANES]
        ok = left > j * LANES
        usable.append(ok)
        keep = -(jnp.maximum(s, 0.0) + jnp.log1p(jnp.exp(-jnp.abs(s))))
        parts.append(jnp.where(ok, keep, 0.0))
    keep = jnp.concatenate(parts, axis=0)
    high = keep.astype(jnp.bfloat16)
    rest = keep - high.astype(jnp.float32)
    mid = rest.astype(jnp.bfloat16)
    low = (rest - mid.astype(jnp.float32)).astype(jnp.bfloat16)
    summed = (
        jnp.dot(low, later_of, preferred_element_type=jnp.float32)
        + jnp.dot(mid, later_of, preferred_element_type=jnp.float32)
        + jnp.dot(high, later_of, preferred_element_type=jnp.float32)
    )
    after = jnp.zeros((seqs, LANES), jnp.float32)
    weights = [None] * chunks
    for j in reversed(range(chunks)):
        s = scores[:, j * LANES : (j + 1) * LANES]
        block = summed[j * seqs : (j + 1) * seqs]
        weights[j] = jnp.where(usable[j], jnp.exp(s + (block[:, :LANES] + after)), 0.0)
        after = after + block[:, LANES:]
    weights = jnp.concatenate(weights, axis=1).astype(jnp.bfloat16)

    for copy in value_loads:
        copy.wait()
    local_out = jnp.zeros((seqs, size), jnp.float32)
    for i in range(pairs):
        rhs = jnp.concatenate([values[2 * i], values[2 * i + 1]], axis=1)
        both = jnp.dot(weights, rhs, preferred_element_type=jnp.float32)
        for k in range(2):
            local_out = jnp.where(qrow == 2 * i + k, both[:, k * size : (k + 1) * size], local_out)

    obuf[me, pl.ds(0, seqs)] = local_out
    obuf[me, pl.ds(seqs, seqs)] = after
    o_push = push("kv", me, n_kv, obuf, o_send, o_recv)
    o_arrival = arrival("kv", me, n_kv, obuf, o_send, o_recv)
    each(n_kv, lambda i: o_push(i).start(), 1)
    each(n_kv, lambda i: o_arrival(i).wait_recv(), 1)

    def combine(i, carry):
        attended, later = carry
        slot = n_kv - 1 - i
        got = obuf[slot]
        return attended + jnp.exp(later) * got[:seqs], later + got[seqs:]

    zero = jnp.zeros((seqs, size), jnp.float32)
    attended, _ = folded(n_kv, combine, (zero, zero))
    mean_sq = jnp.mean(attended * attended, axis=1, keepdims=True)
    normed = (attended * lax.rsqrt(mean_sq + EPS) * hg[...]).astype(jnp.bfloat16)
    columns = wo.shape[1]
    part_out = jnp.dot(normed, wo[...], preferred_element_type=jnp.float32).astype(jnp.bfloat16)
    if columns < tbuf.shape[2]:
        tbuf[mine] = jnp.zeros(tbuf.shape[1:], tbuf.dtype)
    tbuf[mine, :, pl.ds(0, columns)] = part_out
    t_push = push("tp", mine, n_tp, tbuf, t_send, t_recv)
    t_arrival = arrival("tp", mine, n_tp, tbuf, t_send, t_recv)
    each(n_tp, lambda i: t_push(i).start(), 1)
    each(n_tp, lambda i: t_arrival(i).wait_recv(), 1)
    mixed = folded(
        n_tp,
        lambda i, acc: acc + tbuf[i].astype(jnp.float32),
        jnp.zeros(tbuf.shape[1:], jnp.float32),
    )
    out_ref[...] = mixed[:, :columns].astype(out_ref.dtype)

    each(n_kv, lambda i: q_push(i).wait_send(), 1)
    each(n_kv, lambda i: o_push(i).wait_send(), 1)
    each(n_tp, lambda i: t_push(i).wait_send(), 1)


def shards(
    n_kv, n_tp,
    tokens, in_gain, w_query, score_bias, cache_keys, cache_values, lengths, head_gain, w_out,
):
    seqs, local_len, size = cache_keys.shape
    assert score_bias.shape[0] == 1 and seqs % 2 == 0 and local_len % LANES == 0
    columns = w_out.shape[1]
    width = -(-columns // LANES) * LANES
    f32, bf16 = jnp.float32, jnp.bfloat16
    any_space = pl.BlockSpec(memory_space=pl.ANY)
    dma = pltpu.SemaphoreType.DMA
    return pl.pallas_call(
        functools.partial(kernel, n_kv, n_tp),
        out_shape=jax.ShapeDtypeStruct((seqs, columns), bf16),
        in_specs=[any_space] * 9,
        out_specs=pl.BlockSpec(memory_space=pltpu.VMEM),
        scratch_shapes=[
            pltpu.VMEM(tokens.shape, bf16),
            pltpu.VMEM((1, in_gain.shape[0]), f32),
            pltpu.VMEM(w_query.shape, bf16),
            pltpu.SMEM(score_bias.shape, f32),
            pltpu.VMEM(cache_keys.shape, bf16),
            pltpu.VMEM(cache_values.shape, bf16),
            pltpu.SMEM(lengths.shape, jnp.int32),
            pltpu.VMEM((1, head_gain.shape[0]), f32),
            pltpu.VMEM(w_out.shape, bf16),
            pltpu.VMEM((n_kv, 2 * seqs, size), f32),
            pltpu.VMEM((n_kv, 2 * seqs, size), f32),
            pltpu.VMEM((n_tp, seqs, width), bf16),
            dma((7,)),
            dma((seqs // 2,)),
            dma((seqs // 2,)),
            dma((n_kv,)),
            dma((n_kv,)),
            dma((n_kv,)),
            dma((n_kv,)),
            dma((n_tp,)),
            dma((n_tp,)),
        ],
        compiler_params=pltpu.CompilerParams(collective_id=0, has_side_effects=True),
    )(
        tokens, in_gain[None], w_query, score_bias, cache_keys, cache_values, lengths,
        head_gain[None], w_out,
    )


def solution(mesh):
    return jax.shard_map(
        functools.partial(shards, mesh.shape["kv"], mesh.shape["tp"]),
        mesh=mesh,
        in_specs=(
            P(None, "kv"),
            P("kv"),
            P("kv", "tp"),
            P("tp"),
            P(None, "kv", "tp"),
            P(None, "kv", "tp"),
            P(),
            P("tp"),
            P("tp", "kv"),
        ),
        out_specs=P(None, "kv"),
        check_vma=False,
    )
```

```python
import functools

import jax
import jax.numpy as jnp
from jax import lax
from jax.experimental import pallas as pl
from jax.experimental.pallas import tpu as pltpu
from jax.sharding import PartitionSpec as P

EPS = 1e-06
LANES = 128
MESH = pl.DeviceIdType.MESH


def each(count, body, first=0):
    if count - first <= 32:
        for i in range(first, count):
            body(i)
    else:
        lax.fori_loop(first, count, lambda i, c: (body(i), c)[1], 0)


def folded(count, body, init):
    if count <= 32:
        for i in range(count):
            init = body(i, init)
        return init
    return lax.fori_loop(0, count, body, init)


def push(axis, me, count, buf, send_sem, recv_sem, part):
    def copy(i):
        return pltpu.make_async_remote_copy(
            src_ref=part(buf, me),
            dst_ref=part(buf, me),
            send_sem=send_sem.at[i],
            recv_sem=recv_sem.at[i],
            device_id={axis: lax.rem(me + i, count)},
            device_id_type=MESH,
        )

    return copy


def arrival(axis, me, count, buf, send_sem, recv_sem, part):
    def copy(i):
        slot = lax.rem(me + count - i, count)
        return pltpu.make_async_remote_copy(
            src_ref=part(buf, slot),
            dst_ref=part(buf, slot),
            send_sem=send_sem.at[i],
            recv_sem=recv_sem.at[i],
            device_id={axis: slot},
            device_id_type=MESH,
        )

    return copy


def spread(me, mine, n_kv, n_tp, buf, send_sem, recv_sem, rows):
    def copy(n, arriving):
        i, k = n % n_kv, n // n_kv
        if arriving:
            at, beside = lax.rem(me + n_kv - i, n_kv), lax.rem(mine + n_tp - k, n_tp)
        else:
            at, beside = lax.rem(me + i, n_kv), lax.rem(mine + k, n_tp)
        slot = buf.at[beside, at] if arriving else buf.at[mine, me]
        return pltpu.make_async_remote_copy(
            src_ref=slot.at[pl.ds(0, rows)],
            dst_ref=slot.at[pl.ds(0, rows)],
            send_sem=send_sem.at[n],
            recv_sem=recv_sem.at[n],
            device_id={"kv": at, "tp": beside},
            device_id_type=MESH,
        )

    return copy


def kernel(
    n_kv, n_tp,
    tok_hbm, gain_hbm, wq_hbm, bias_hbm, keys_hbm, values_hbm, len_hbm, hg_hbm, wo_hbm,
    out_ref,
    tok, gain, wq, bias, keys, values, lens, hg, wo,
    qbuf, obuf,
    load_sem, key_sem, value_sem,
    q_send, q_recv, o_send, o_recv, w_send, w_recv, h_send, h_recv,
):
    me = lax.axis_index("kv")
    mine = lax.axis_index("tp")
    seqs, local_len, size = keys.shape
    chunks = local_len // LANES

    small = [
        pltpu.make_async_copy(src, dst, load_sem.at[i])
        for i, (src, dst) in enumerate(
            ((tok_hbm, tok), (gain_hbm, gain), (wq_hbm, wq), (bias_hbm, bias),
             (len_hbm, lens), (hg_hbm, hg.at[mine]), (wo_hbm, wo.at[mine]))
        )
    ]
    for copy in small:
        copy.start()
    barrier = pltpu.get_barrier_semaphore()

    def greet(axis, place, count):
        def body(i):
            pl.semaphore_signal(
                barrier, inc=1, device_id={axis: lax.rem(place + i, count)}, device_id_type=MESH
            )

        each(count, body, 1)

    greet("kv", me, n_kv)
    greet("tp", mine, n_tp)
    devices = n_kv * n_tp
    pairs = seqs // 2
    key_loads = [
        pltpu.make_async_copy(
            keys_hbm.at[pl.ds(2 * i, 2)], keys.at[pl.ds(2 * i, 2)], key_sem.at[i]
        )
        for i in range(pairs)
    ]
    value_loads = [
        pltpu.make_async_copy(
            values_hbm.at[pl.ds(2 * i, 2)], values.at[pl.ds(2 * i, 2)], value_sem.at[i]
        )
        for i in range(pairs)
    ]
    for copy in key_loads + value_loads:
        copy.start()

    for copy in small[:3]:
        copy.wait()
    as_float = tok[...].astype(jnp.float32)
    gained = (as_float * gain[...]).astype(jnp.bfloat16)
    partial = jnp.dot(gained, wq[...], preferred_element_type=jnp.float32)
    squares = jnp.sum(as_float * as_float, axis=1, keepdims=True)
    row = lax.broadcasted_iota(jnp.int32, (seqs, LANES), 0)
    lane = lax.broadcasted_iota(jnp.int32, (seqs, LANES), 1)
    diagonal = row == lane
    qbuf[me, pl.ds(0, seqs)] = partial
    qbuf[me, pl.ds(seqs, 1)] = jnp.sum(jnp.where(diagonal, squares, 0.0), axis=0, keepdims=True)
    pl.semaphore_wait(barrier, n_kv - 1 + n_tp - 1)

    def q_part(buf, slot):
        return buf.at[slot, pl.ds(0, seqs + 1)]

    q_push = push("kv", me, n_kv, qbuf, q_send, q_recv, q_part)
    q_arrival = arrival("kv", me, n_kv, qbuf, q_send, q_recv, q_part)
    each(n_kv, lambda i: q_push(i).start(), 1)

    for copy in small[3:]:
        copy.wait()

    def whole(buf, slot):
        return buf.at[slot]

    w_push = push("tp", mine, n_tp, wo, w_send, w_recv, whole)
    w_arrival = arrival("tp", mine, n_tp, wo, w_send, w_recv, whole)
    h_push = push("tp", mine, n_tp, hg, h_send, h_recv, whole)
    h_arrival = arrival("tp", mine, n_tp, hg, h_send, h_recv, whole)
    each(n_tp, lambda i: w_push(i).start(), 1)
    each(n_tp, lambda i: h_push(i).start(), 1)
    length = jnp.zeros((seqs, LANES), jnp.int32)
    for b in range(seqs):
        length = jnp.where(row == b, lens[b], length)
    left = length - (me * local_len + lane)
    shift = bias[0]
    from_row = lax.broadcasted_iota(jnp.int32, (LANES, 2 * LANES), 0)
    to_lane = lax.broadcasted_iota(jnp.int32, (LANES, 2 * LANES), 1)
    later_of = jnp.where((from_row >= to_lane) | (to_lane >= LANES), 1.0, 0.0).astype(jnp.bfloat16)
    for copy in key_loads:
        copy.wait()

    each(n_kv, lambda i: q_arrival(i).wait_recv(), 1)
    total, squares = folded(
        n_kv,
        lambda i, acc: (acc[0] + qbuf[i, pl.ds(0, seqs)], acc[1] + qbuf[i, pl.ds(seqs, 1)]),
        (jnp.zeros((seqs, size), jnp.float32), jnp.zeros((1, size), jnp.float32)),
    )
    squares = jnp.sum(jnp.where(diagonal, squares, 0.0), axis=1, keepdims=True)
    features = tok.shape[1] * n_kv
    row_scale = lax.rsqrt(squares / features + EPS)
    queries = total * row_scale
    queries = queries.astype(jnp.bfloat16).astype(jnp.float32)
    qrow = lax.broadcasted_iota(jnp.int32, (seqs, size), 0)

    scores = None
    for i in range(pairs):
        lhs = jnp.concatenate(
            [jnp.where(qrow == 2 * i + k, queries, 0.0) for k in range(2)], axis=1
        ).astype(jnp.bfloat16)
        rhs = jnp.concatenate([keys[2 * i], keys[2 * i + 1]], axis=1)
        term = lax.dot_general(
            lhs, rhs, (((1,), (1,)), ((), ())), preferred_element_type=jnp.float32
        )
        scores = term if scores is None else scores + term
    scores = scores * size ** (-0.5) + shift

    usable, parts = [], []
    for j in range(chunks):
        s = scores[:, j * LANES : (j + 1) * LANES]
        ok = left > j * LANES
        usable.append(ok)
        keep = -(jnp.maximum(s, 0.0) + jnp.log1p(jnp.exp(-jnp.abs(s))))
        parts.append(jnp.where(ok, keep, 0.0))
    keep = jnp.concatenate(parts, axis=0)
    high = keep.astype(jnp.bfloat16)
    rest = keep - high.astype(jnp.float32)
    mid = rest.astype(jnp.bfloat16)
    low = (rest - mid.astype(jnp.float32)).astype(jnp.bfloat16)
    summed = (
        jnp.dot(low, later_of, preferred_element_type=jnp.float32)
        + jnp.dot(mid, later_of, preferred_element_type=jnp.float32)
        + jnp.dot(high, later_of, preferred_element_type=jnp.float32)
    )
    after = jnp.zeros((seqs, LANES), jnp.float32)
    weights = [None] * chunks
    for j in reversed(range(chunks)):
        s = scores[:, j * LANES : (j + 1) * LANES]
        block = summed[j * seqs : (j + 1) * seqs]
        weights[j] = jnp.where(usable[j], jnp.exp(s + (block[:, :LANES] + after)), 0.0)
        after = after + block[:, LANES:]
    weights = jnp.concatenate(weights, axis=1).astype(jnp.bfloat16)

    for copy in value_loads:
        copy.wait()
    local_out = jnp.zeros((seqs, size), jnp.float32)
    for i in range(pairs):
        rhs = jnp.concatenate([values[2 * i], values[2 * i + 1]], axis=1)
        both = jnp.dot(weights, rhs, preferred_element_type=jnp.float32)
        for k in range(2):
            local_out = jnp.where(qrow == 2 * i + k, both[:, k * size : (k + 1) * size], local_out)

    after = jnp.sum(jnp.where(diagonal, after, 0.0), axis=0, keepdims=True)
    first = after.astype(jnp.bfloat16).astype(jnp.float32)
    second = (after - first).astype(jnp.bfloat16).astype(jnp.float32)
    third = after - first - second
    tail = jnp.where(row == 0, first, jnp.where(row == 1, second, jnp.where(row == 2, third, 0.0)))
    obuf[mine, me] = jnp.concatenate([local_out, tail], axis=0).astype(jnp.bfloat16)
    spreading = spread(me, mine, n_kv, n_tp, obuf, o_send, o_recv, seqs + 4)
    each(devices, lambda n: spreading(n, False).start(), 1)
    each(n_tp, lambda i: w_arrival(i).wait_recv(), 1)
    each(n_tp, lambda i: h_arrival(i).wait_recv(), 1)
    each(devices, lambda n: spreading(n, True).wait_recv(), 1)

    mixed = None
    for t in range(n_tp):

        def combine(i, carry):
            attended, later = carry
            slot = n_kv - 1 - i
            got = obuf[t, slot].astype(jnp.float32)
            scale = jnp.sum(jnp.where(diagonal, jnp.exp(later), 0.0), axis=1, keepdims=True)
            later = later + (got[seqs : seqs + 1] + got[seqs + 1 : seqs + 2] + got[seqs + 2 : seqs + 3])
            return attended + scale * got[:seqs], later

        attended, _ = folded(
            n_kv,
            combine,
            (jnp.zeros((seqs, size), jnp.float32), jnp.zeros((1, LANES), jnp.float32)),
        )
        mean_sq = jnp.mean(attended * attended, axis=1, keepdims=True)
        normed = (attended * lax.rsqrt(mean_sq + EPS) * hg[t]).astype(jnp.bfloat16)
        part_out = jnp.dot(normed, wo[t], preferred_element_type=jnp.float32)
        part_out = part_out.astype(jnp.bfloat16).astype(jnp.float32)
        mixed = part_out if mixed is None else mixed + part_out
    out_ref[...] = mixed.astype(out_ref.dtype)

    each(n_kv, lambda i: q_push(i).wait_send(), 1)
    each(n_tp, lambda i: w_push(i).wait_send(), 1)
    each(n_tp, lambda i: h_push(i).wait_send(), 1)
    each(devices, lambda n: spreading(n, False).wait_send(), 1)


def shards(
    n_kv, n_tp,
    tokens, in_gain, w_query, score_bias, cache_keys, cache_values, lengths, head_gain, w_out,
):
    seqs, local_len, size = cache_keys.shape
    assert score_bias.shape[0] == 1 and seqs % 2 == 0 and local_len % LANES == 0
    columns = w_out.shape[1]
    f32, bf16 = jnp.float32, jnp.bfloat16
    any_space = pl.BlockSpec(memory_space=pl.ANY)
    dma = pltpu.SemaphoreType.DMA
    return pl.pallas_call(
        functools.partial(kernel, n_kv, n_tp),
        out_shape=jax.ShapeDtypeStruct((seqs, columns), bf16),
        in_specs=[any_space] * 9,
        out_specs=pl.BlockSpec(memory_space=pltpu.VMEM),
        scratch_shapes=[
            pltpu.VMEM(tokens.shape, bf16),
            pltpu.VMEM((1, in_gain.shape[0]), f32),
            pltpu.VMEM(w_query.shape, bf16),
            pltpu.SMEM(score_bias.shape, f32),
            pltpu.VMEM(cache_keys.shape, bf16),
            pltpu.VMEM(cache_values.shape, bf16),
            pltpu.SMEM(lengths.shape, jnp.int32),
            pltpu.VMEM((n_tp, 1, size), f32),
            pltpu.VMEM((n_tp, *w_out.shape), bf16),
            pltpu.VMEM((n_kv, 2 * seqs, size), f32),
            pltpu.VMEM((n_tp, n_kv, 2 * seqs, size), bf16),
            dma((7,)),
            dma((seqs // 2,)),
            dma((seqs // 2,)),
            dma((n_kv,)),
            dma((n_kv,)),
            dma((n_kv * n_tp,)),
            dma((n_kv * n_tp,)),
            dma((n_tp,)),
            dma((n_tp,)),
            dma((n_tp,)),
            dma((n_tp,)),
        ],
        compiler_params=pltpu.CompilerParams(collective_id=0, has_side_effects=True),
    )(
        tokens, in_gain[None], w_query, score_bias, cache_keys, cache_values, lengths,
        head_gain[None], w_out,
    )


def solution(mesh):
    return jax.shard_map(
        functools.partial(shards, mesh.shape["kv"], mesh.shape["tp"]),
        mesh=mesh,
        in_specs=(
            P(None, "kv"),
            P("kv"),
            P("kv", "tp"),
            P("tp"),
            P(None, "kv", "tp"),
            P(None, "kv", "tp"),
            P(),
            P("tp"),
            P("tp", "kv"),
        ),
        out_specs=P(None, "kv"),
        check_vma=False,
    )
```

```python
import functools

import jax
import jax.numpy as jnp
from jax import lax
from jax.experimental import pallas as pl
from jax.experimental.pallas import tpu as pltpu
from jax.sharding import PartitionSpec as P

EPS = 1e-06
LANES = 128
MESH = pl.DeviceIdType.MESH


def each(count, body, first=0):
    if count - first <= 32:
        for i in range(first, count):
            body(i)
    else:
        lax.fori_loop(first, count, lambda i, c: (body(i), c)[1], 0)


def folded(count, body, init):
    if count <= 32:
        for i in range(count):
            init = body(i, init)
        return init
    return lax.fori_loop(0, count, body, init)


def push(axis, me, count, buf, send_sem, recv_sem, part):
    def copy(i):
        return pltpu.make_async_remote_copy(
            src_ref=part(buf, me),
            dst_ref=part(buf, me),
            send_sem=send_sem.at[i],
            recv_sem=recv_sem.at[i],
            device_id={axis: lax.rem(me + i, count)},
            device_id_type=MESH,
        )

    return copy


def arrival(axis, me, count, buf, send_sem, recv_sem, part):
    def copy(i):
        slot = lax.rem(me + count - i, count)
        return pltpu.make_async_remote_copy(
            src_ref=part(buf, slot),
            dst_ref=part(buf, slot),
            send_sem=send_sem.at[i],
            recv_sem=recv_sem.at[i],
            device_id={axis: slot},
            device_id_type=MESH,
        )

    return copy


def spread(me, mine, n_kv, n_tp, buf, send_sem, recv_sem, rows):
    def copy(n, arriving):
        i, k = n % n_kv, n // n_kv
        if arriving:
            at, beside = lax.rem(me + n_kv - i, n_kv), lax.rem(mine + n_tp - k, n_tp)
        else:
            at, beside = lax.rem(me + i, n_kv), lax.rem(mine + k, n_tp)
        slot = buf.at[beside, at] if arriving else buf.at[mine, me]
        return pltpu.make_async_remote_copy(
            src_ref=slot.at[pl.ds(0, rows)],
            dst_ref=slot.at[pl.ds(0, rows)],
            send_sem=send_sem.at[n],
            recv_sem=recv_sem.at[n],
            device_id={"kv": at, "tp": beside},
            device_id_type=MESH,
        )

    return copy


def kernel(
    n_kv, n_tp,
    tok_hbm, gain_hbm, wq_hbm, bias_hbm, keys_hbm, values_hbm, len_hbm, hg_hbm, wo_hbm,
    out_ref,
    tok, gain, wq, bias, keys, values, lens, hg, wo,
    qbuf, obuf,
    load_sem, key_sem, value_sem,
    q_send, q_recv, o_send, o_recv, w_send, w_recv, h_send, h_recv,
):
    me = lax.axis_index("kv")
    mine = lax.axis_index("tp")
    seqs, local_len, size = keys.shape
    chunks = local_len // LANES

    small = [
        pltpu.make_async_copy(src, dst, load_sem.at[i])
        for i, (src, dst) in enumerate(
            ((tok_hbm, tok), (gain_hbm, gain), (wq_hbm, wq), (bias_hbm, bias),
             (len_hbm, lens), (hg_hbm, hg.at[mine]), (wo_hbm, wo.at[mine]))
        )
    ]
    barrier = pltpu.get_barrier_semaphore()

    def greet(axis, place, count):
        def body(i):
            pl.semaphore_signal(
                barrier, inc=1, device_id={axis: lax.rem(place + i, count)}, device_id_type=MESH
            )

        each(count, body, 1)

    greet("kv", me, n_kv)
    greet("tp", mine, n_tp)
    devices = n_kv * n_tp
    for copy in small:
        copy.start()
    pairs = seqs // 2
    key_loads = [
        pltpu.make_async_copy(
            keys_hbm.at[pl.ds(2 * i, 2)], keys.at[pl.ds(2 * i, 2)], key_sem.at[i]
        )
        for i in range(pairs)
    ]
    value_loads = [
        pltpu.make_async_copy(
            values_hbm.at[pl.ds(2 * i, 2)], values.at[pl.ds(2 * i, 2)], value_sem.at[i]
        )
        for i in range(pairs)
    ]
    for copy in key_loads + value_loads:
        copy.start()

    for copy in small[:3]:
        copy.wait()
    as_float = tok[...].astype(jnp.float32)
    gained = (as_float * gain[...]).astype(jnp.bfloat16)
    partial = jnp.dot(gained, wq[...], preferred_element_type=jnp.float32)
    squares = jnp.sum(as_float * as_float, axis=1, keepdims=True)
    row = lax.broadcasted_iota(jnp.int32, (seqs, LANES), 0)
    lane = lax.broadcasted_iota(jnp.int32, (seqs, LANES), 1)
    diagonal = row == lane
    qbuf[me, pl.ds(0, seqs)] = partial
    qbuf[me, pl.ds(seqs, 1)] = jnp.sum(jnp.where(diagonal, squares, 0.0), axis=0, keepdims=True)
    pl.semaphore_wait(barrier, n_kv - 1 + n_tp - 1)

    def q_part(buf, slot):
        return buf.at[slot, pl.ds(0, seqs + 1)]

    q_push = push("kv", me, n_kv, qbuf, q_send, q_recv, q_part)
    q_arrival = arrival("kv", me, n_kv, qbuf, q_send, q_recv, q_part)
    each(n_kv, lambda i: q_push(n_kv - i).start(), 1)

    for copy in small[3:]:
        copy.wait()

    def whole(buf, slot):
        return buf.at[slot]

    w_push = push("tp", mine, n_tp, wo, w_send, w_recv, whole)
    w_arrival = arrival("tp", mine, n_tp, wo, w_send, w_recv, whole)
    h_push = push("tp", mine, n_tp, hg, h_send, h_recv, whole)
    h_arrival = arrival("tp", mine, n_tp, hg, h_send, h_recv, whole)
    each(n_tp, lambda i: w_push(i).start(), 1)
    each(n_tp, lambda i: h_push(i).start(), 1)
    length = jnp.zeros((seqs, LANES), jnp.int32)
    for b in range(seqs):
        length = jnp.where(row == b, lens[b], length)
    left = length - (me * local_len + lane)
    shift = bias[0]
    from_row = lax.broadcasted_iota(jnp.int32, (LANES, 2 * LANES), 0)
    to_lane = lax.broadcasted_iota(jnp.int32, (LANES, 2 * LANES), 1)
    later_of = jnp.where((from_row >= to_lane) | (to_lane >= LANES), 1.0, 0.0).astype(jnp.bfloat16)
    for copy in key_loads:
        copy.wait()

    each(n_kv, lambda i: q_arrival(i).wait_recv(), 1)
    total, squares = folded(
        n_kv,
        lambda i, acc: (acc[0] + qbuf[i, pl.ds(0, seqs)], acc[1] + qbuf[i, pl.ds(seqs, 1)]),
        (jnp.zeros((seqs, size), jnp.float32), jnp.zeros((1, size), jnp.float32)),
    )
    squares = jnp.sum(jnp.where(diagonal, squares, 0.0), axis=1, keepdims=True)
    features = tok.shape[1] * n_kv
    row_scale = lax.rsqrt(squares / features + EPS)
    queries = total * row_scale
    queries = queries.astype(jnp.bfloat16).astype(jnp.float32)
    qrow = lax.broadcasted_iota(jnp.int32, (seqs, size), 0)

    scores = None
    for i in range(pairs):
        lhs = jnp.concatenate(
            [jnp.where(qrow == 2 * i + k, queries, 0.0) for k in range(2)], axis=1
        ).astype(jnp.bfloat16)
        rhs = jnp.concatenate([keys[2 * i], keys[2 * i + 1]], axis=1)
        term = lax.dot_general(
            lhs, rhs, (((1,), (1,)), ((), ())), preferred_element_type=jnp.float32
        )
        scores = term if scores is None else scores + term
    scores = scores * size ** (-0.5) + shift

    usable, parts = [], []
    for j in range(chunks):
        s = scores[:, j * LANES : (j + 1) * LANES]
        ok = left > j * LANES
        usable.append(ok)
        keep = -(jnp.maximum(s, 0.0) + jnp.log1p(jnp.exp(-jnp.abs(s))))
        parts.append(jnp.where(ok, keep, 0.0))
    keep = jnp.concatenate(parts, axis=0)
    high = keep.astype(jnp.bfloat16)
    rest = keep - high.astype(jnp.float32)
    mid = rest.astype(jnp.bfloat16)
    low = (rest - mid.astype(jnp.float32)).astype(jnp.bfloat16)
    summed = (
        jnp.dot(low, later_of, preferred_element_type=jnp.float32)
        + jnp.dot(mid, later_of, preferred_element_type=jnp.float32)
        + jnp.dot(high, later_of, preferred_element_type=jnp.float32)
    )
    after = jnp.zeros((seqs, LANES), jnp.float32)
    weights = [None] * chunks
    for j in reversed(range(chunks)):
        s = scores[:, j * LANES : (j + 1) * LANES]
        block = summed[j * seqs : (j + 1) * seqs]
        weights[j] = jnp.where(usable[j], jnp.exp(s + (block[:, :LANES] + after)), 0.0)
        after = after + block[:, LANES:]
    weights = jnp.concatenate(weights, axis=1).astype(jnp.bfloat16)

    for copy in value_loads:
        copy.wait()
    local_out = jnp.zeros((seqs, size), jnp.float32)
    for i in range(pairs):
        rhs = jnp.concatenate([values[2 * i], values[2 * i + 1]], axis=1)
        both = jnp.dot(weights, rhs, preferred_element_type=jnp.float32)
        for k in range(2):
            local_out = jnp.where(qrow == 2 * i + k, both[:, k * size : (k + 1) * size], local_out)

    after = jnp.sum(jnp.where(diagonal, after, 0.0), axis=0, keepdims=True)
    first = after.astype(jnp.bfloat16).astype(jnp.float32)
    second = (after - first).astype(jnp.bfloat16).astype(jnp.float32)
    third = after - first - second
    tail = jnp.where(row == 0, first, jnp.where(row == 1, second, jnp.where(row == 2, third, 0.0)))
    obuf[mine, me] = jnp.concatenate([local_out, tail], axis=0).astype(jnp.bfloat16)
    spreading = spread(me, mine, n_kv, n_tp, obuf, o_send, o_recv, seqs + 4)
    each(devices, lambda n: spreading(n, False).start(), 1)
    each(n_tp, lambda i: w_arrival(i).wait_recv(), 1)
    each(n_tp, lambda i: h_arrival(i).wait_recv(), 1)
    each(devices, lambda n: spreading(n, True).wait_recv(), 1)

    mixed = None
    for t in range(n_tp):

        def combine(i, carry):
            attended, later = carry
            slot = n_kv - 1 - i
            got = obuf[t, slot].astype(jnp.float32)
            scale = jnp.sum(jnp.where(diagonal, jnp.exp(later), 0.0), axis=1, keepdims=True)
            later = later + (got[seqs : seqs + 1] + got[seqs + 1 : seqs + 2] + got[seqs + 2 : seqs + 3])
            return attended + scale * got[:seqs], later

        attended, _ = folded(
            n_kv,
            combine,
            (jnp.zeros((seqs, size), jnp.float32), jnp.zeros((1, LANES), jnp.float32)),
        )
        mean_sq = jnp.mean(attended * attended, axis=1, keepdims=True)
        normed = (attended * lax.rsqrt(mean_sq + EPS) * hg[t]).astype(jnp.bfloat16)
        part_out = jnp.dot(normed, wo[t], preferred_element_type=jnp.float32)
        part_out = part_out.astype(jnp.bfloat16).astype(jnp.float32)
        mixed = part_out if mixed is None else mixed + part_out
    out_ref[...] = mixed.astype(out_ref.dtype)

    each(n_kv, lambda i: q_push(i).wait_send(), 1)
    each(n_tp, lambda i: w_push(i).wait_send(), 1)
    each(n_tp, lambda i: h_push(i).wait_send(), 1)
    each(devices, lambda n: spreading(n, False).wait_send(), 1)


def shards(
    n_kv, n_tp,
    tokens, in_gain, w_query, score_bias, cache_keys, cache_values, lengths, head_gain, w_out,
):
    seqs, local_len, size = cache_keys.shape
    assert score_bias.shape[0] == 1 and seqs % 2 == 0 and local_len % LANES == 0
    columns = w_out.shape[1]
    f32, bf16 = jnp.float32, jnp.bfloat16
    any_space = pl.BlockSpec(memory_space=pl.ANY)
    dma = pltpu.SemaphoreType.DMA
    return pl.pallas_call(
        functools.partial(kernel, n_kv, n_tp),
        out_shape=jax.ShapeDtypeStruct((seqs, columns), bf16),
        in_specs=[any_space] * 9,
        out_specs=pl.BlockSpec(memory_space=pltpu.VMEM),
        scratch_shapes=[
            pltpu.VMEM(tokens.shape, bf16),
            pltpu.VMEM((1, in_gain.shape[0]), f32),
            pltpu.VMEM(w_query.shape, bf16),
            pltpu.SMEM(score_bias.shape, f32),
            pltpu.VMEM(cache_keys.shape, bf16),
            pltpu.VMEM(cache_values.shape, bf16),
            pltpu.SMEM(lengths.shape, jnp.int32),
            pltpu.VMEM((n_tp, 1, size), f32),
            pltpu.VMEM((n_tp, *w_out.shape), bf16),
            pltpu.VMEM((n_kv, 2 * seqs, size), f32),
            pltpu.VMEM((n_tp, n_kv, 2 * seqs, size), bf16),
            dma((7,)),
            dma((seqs // 2,)),
            dma((seqs // 2,)),
            dma((n_kv,)),
            dma((n_kv,)),
            dma((n_kv * n_tp,)),
            dma((n_kv * n_tp,)),
            dma((n_tp,)),
            dma((n_tp,)),
            dma((n_tp,)),
            dma((n_tp,)),
        ],
        compiler_params=pltpu.CompilerParams(collective_id=0, has_side_effects=True),
    )(
        tokens, in_gain[None], w_query, score_bias, cache_keys, cache_values, lengths,
        head_gain[None], w_out,
    )


def solution(mesh):
    return jax.shard_map(
        functools.partial(shards, mesh.shape["kv"], mesh.shape["tp"]),
        mesh=mesh,
        in_specs=(
            P(None, "kv"),
            P("kv"),
            P("kv", "tp"),
            P("tp"),
            P(None, "kv", "tp"),
            P(None, "kv", "tp"),
            P(),
            P("tp"),
            P("tp", "kv"),
        ),
        out_specs=P(None, "kv"),
        check_vma=False,
    )
```
